32 devices in a mesh: sp: 8 (over z, x), tp: 4 (over y, core).
Axes of the slice: x: 2, y: 2, z: 4, core: 2. Of those that a mesh axis runs over, the one named last changes fastest.
Arguments:
- queries: bfloat16 [4096, 512], P('sp', 'tp'), may hold values from -9.5625 to 9.5625
- keys: bfloat16 [4096, 512], P('sp', 'tp'), may hold values from -9.5625 to 9.5625
- values: bfloat16 [4096, 512], P('sp', 'tp'), may hold values from -6 to 6
- key_bias: bfloat16 [4096, 8], P('sp', 'tp'), may hold values from -17 to 0
- residual: bfloat16 [4096, 2048], P(('sp', 'tp')), may hold values from -6 to 6
- out_weight: bfloat16 [512, 2048], replicated, may hold values from -1 to 1
- norm_gain: float32 [2048], replicated, may hold values from 0.1 to 1.9
- routes: int32 [4096, 2], P(('sp', 'tp')), may hold values from 0 to 7, all different within a row; in each aligned block of 128 rows (0 to 127, 128 to 255, ...) at most 40 rows name the same one
- route_weights: float32 [4096, 2], P(('sp', 'tp')), may hold values from 0.25 to 2
- gate_weight: bfloat16 [8, 2048, 4096], P('sp', None, 'tp'), may hold values from -0.125 to 0.125
- up_weight: bfloat16 [8, 2048, 4096], P('sp', None, 'tp'), may hold values from -0.125 to 0.125
- down_weight: bfloat16 [8, 4096, 2048], P('sp', 'tp'), may hold values from -0.09375 to 0.09375
Outputs:
- output: bfloat16 [4096, 2048], P(('sp', 'tp'))
The draws below stay inside these ranges and needn't reach their ends.
Inputs may be any that keep to these rules, and one draw needn't show every extreme that they name: `routes`: each row names 2 different experts; the rows of one device name no expert more than 40 times.
All inputs are finite; a program needn't handle non-finite values.
Results may differ from the reference program's by a relative error of at most 0.017.
Values may be sent and summed in bfloat16 or wider, within the bound.
A program may use at most 128 MiB of HBM per device.

```python
import math
import jax
import jax.numpy as jnp
import numpy as np
from jax import lax

D = 2048
HEAD_COUNT = 8
HEAD_DIM = 64
FF = 4096
TOP = 2
SPAN = 512
TOK_DEV = 128
TOK_SP = 512
SEQUENCE_LENGTH = 4096
EXPERTS = 8
CAP = 40
N_SP = 8
N_TP = 4


def draw_key_bias(key, part):
    gathered_keys = jax.random.split(jax.random.fold_in(key, 7), 6)
    fast_share = 0.5
    is_fast = jax.random.uniform(gathered_keys[0], (HEAD_COUNT,), jnp.float32) < fast_share
    slow_level = -jnp.log(jnp.float32(SEQUENCE_LENGTH)) - 3.0 + jax.random.uniform(gathered_keys[1], (HEAD_COUNT,), jnp.float32, minval=-0.5, maxval=0.5)
    fast_level = jax.random.uniform(gathered_keys[2], (HEAD_COUNT,), jnp.float32, minval=-7.0, maxval=-5.5)
    level = jnp.where(is_fast, fast_level, slow_level)
    block_shift = jnp.repeat(jax.random.uniform(gathered_keys[3], (N_SP,), jnp.float32, minval=-0.7, maxval=0.7), TOK_SP, total_repeat_length=SEQUENCE_LENGTH)
    sudden_position = jax.random.randint(gathered_keys[4], (4,), 0, SEQUENCE_LENGTH)
    sudden_value = jax.random.uniform(gathered_keys[5], (4, HEAD_COUNT), jnp.float32, minval=-1.5, maxval=0.0)
    position_index = jnp.arange(SEQUENCE_LENGTH, dtype=jnp.int32)
    sudden_hit_mask = (position_index[:, None] == sudden_position[None, :]).astype(jnp.float32)
    any_hit_flag = jnp.sum(sudden_hit_mask, axis=1, keepdims=True) > 0.0
    sudden_rows = jnp.dot(sudden_hit_mask, sudden_value)
    regular_rows = level[None, :] + block_shift[:, None]
    return jnp.where(any_hit_flag, sudden_rows, regular_rows).astype(jnp.bfloat16)


def levels(key, extent, pieces, smallest, high):
    factor_of = 1.0
    for position, shards_of in pieces:
        steps = jax.random.uniform(jax.random.fold_in(jax.random.fold_in(key, 6), position), (shards_of,), jnp.float32, smallest / len(pieces), high / len(pieces))
        factor_of = factor_of * jnp.repeat(jnp.exp(steps), extent[position] // shards_of).reshape((-1,) + (1,) * (len(extent) - 1 - position))
    return factor_of


def shared_out(own_key, own, number, rows, number_of, top, most, lean):
    ranking = jax.random.permutation(own_key, number_of)
    crowded, ordinary = load_shares(number_of, rows * top, most, lean, True), load_shares(number_of, rows * top, most, lean, False)
    places = jnp.arange(number_of)

    def named(lengths, offset_by):
        used = int((lengths > 0).sum())
        fixed = max(1, used // 4)
        shifted = fixed + (places - fixed + offset_by * (used - fixed)) % max(1, number_of - fixed)
        return jnp.zeros((number_of,), jnp.int32).at[ranking[jnp.where(places < fixed, places, shifted)]].set(jnp.asarray(lengths, jnp.int32))

    lengths = jnp.where(number % 4 == 0, named(crowded, number // 4), named(ordinary, number - number // 4 - 1))
    mixed = jax.random.permutation(jax.random.fold_in(own, 3), number_of)
    source_of, taker = mixed[0:number_of // 2 * 2:2], mixed[1:number_of // 2 * 2:2]
    room = jnp.minimum(lengths[source_of] - 1, most - lengths[taker]) // 2
    room = jnp.where((source_of == ranking[0]) | (taker == ranking[0]) | (lengths[taker] == 0), 0, jnp.maximum(room, 0))
    shifted = jax.random.randint(jax.random.fold_in(own, 4), (number_of // 2,), 0, 1 << 20) % (room + 1)
    lengths = lengths.at[source_of].add(-shifted).at[taker].add(shifted)
    labels = jnp.searchsorted(jnp.cumsum(lengths), jnp.arange(rows * top), side="right").astype(jnp.int32)
    table = labels.reshape(top, rows).T
    table = table[jax.random.permutation(jax.random.fold_in(own, 1), rows)]
    offset_by = jax.random.randint(jax.random.fold_in(own, 2), (rows, 1), 0, top)
    return jnp.take_along_axis(table, (jnp.arange(top)[None, :] + offset_by) % top, axis=1)


def load_shares(amount, total, reach, slope, full):
    portions = [(1 << 20) // math.isqrt(rank ** slope) + 1 for rank in range(1, amount + 1)]
    largest = reach if full else min(reach, max(-(-total // amount), total * portions[0] // sum(portions)))
    least = 1 if total - largest >= amount - 1 else 0
    given, rest = [largest] + [least] * (amount - 1), total - largest - least * (amount - 1)
    while rest > 0:
        candidates = [i for i in range(1, amount) if given[i] < largest] or [i for i in range(1, amount) if given[i] < reach]
        whole, left = sum([portions[i] for i in candidates]), rest
        for i in candidates:
            more = min(reach - given[i], max(1, left * portions[i] // whole), rest)
            given[i] = given[i] + more
            rest = rest - more
    return np.array(given)


def normal_values(rng, shape, width, bound, pieces=(), held_as=jnp.bfloat16):
    result = jax.random.normal(rng, shape, jnp.float32) * width
    if len(pieces) > 0:
        result = levels(rng, shape, pieces, -0.22, 0.18) * result
    return jnp.clip(result, min=-bound, max=bound).astype(held_as)


def setup_inputs(seed: int = 0) -> dict:
    splits = jax.random.split(jax.random.key(seed), 13)
    queries = normal_values(splits[0], (SEQUENCE_LENGTH, HEAD_COUNT * HEAD_DIM), 1.6, 9.5625, ((0, 8), (1, 4)))
    keys = normal_values(splits[1], (SEQUENCE_LENGTH, HEAD_COUNT * HEAD_DIM), 1.6, 9.5625, ((0, 8), (1, 4)))
    values = normal_values(splits[2], (SEQUENCE_LENGTH, HEAD_COUNT * HEAD_DIM), 1.0, 6.0, ((0, 8), (1, 4)))
    key_bias = draw_key_bias(jax.random.fold_in(splits[12], 71), 0)
    residual = normal_values(splits[4], (SEQUENCE_LENGTH, D), 1.0, 6.0, ((0, 32),))
    out_weight = normal_values(splits[5], (HEAD_COUNT * HEAD_DIM, D), (HEAD_COUNT * HEAD_DIM // 16) ** -0.5, 1.0)
    norm_gain = jnp.clip(1.0 + 0.18 * jax.random.normal(splits[6], (D,), jnp.float32), 0.1, 1.9)
    routes_keys = jax.random.split(jax.random.fold_in(splits[7], 1), SEQUENCE_LENGTH // TOK_DEV)
    routes_turns = jax.random.permutation(jax.random.fold_in(splits[7], 3), SEQUENCE_LENGTH // TOK_DEV)
    routes = jax.vmap(lambda own, number: shared_out(jax.random.fold_in(splits[7], 2), own, number, TOK_DEV, EXPERTS, TOP, CAP, 1))(routes_keys, routes_turns).reshape((SEQUENCE_LENGTH, TOP))
    route_weights = jnp.clip(jnp.exp(math.log(2.0) - 2.0794415 * jax.random.uniform(splits[8], (SEQUENCE_LENGTH, TOP), jnp.float32) ** levels(splits[8], (SEQUENCE_LENGTH, TOP), ((0, 32),), -0.2, 0.2)), 0.25, 2.0)
    gate_weight = normal_values(splits[9], (EXPERTS, D, FF), D ** -0.5, 0.125, ((0, 8), (2, 4)))
    up_weight = normal_values(splits[10], (EXPERTS, D, FF), D ** -0.5, 0.125, ((0, 8), (2, 4)))
    down_weight = normal_values(splits[11], (EXPERTS, FF, D), FF ** -0.5, 0.09375, ((0, 8), (1, 4)))
    return {"queries": queries, "keys": keys, "values": values, "key_bias": key_bias, "residual": residual, "out_weight": out_weight, "norm_gain": norm_gain, "routes": routes, "route_weights": route_weights, "gate_weight": gate_weight, "up_weight": up_weight, "down_weight": down_weight}


epsilon = 1e-06

def stick_span(query_block, key_block, value_block, bias_block, query_pos, key_pos):
    scores = jnp.einsum('qhd,khd->qhk', query_block, key_block) * HEAD_DIM ** (-0.5)
    scores = scores + jnp.transpose(bias_block)[None, :, :]
    earlier = key_pos[None, None, :] < query_pos[:, None, None]
    failure = jnp.where(earlier, jax.nn.log_sigmoid(-scores), 0.0)
    later_sum = lax.cumsum(failure, axis=2, reverse=True) - failure
    weights = jnp.where(earlier, jnp.exp(jax.nn.log_sigmoid(scores) + later_sum), 0.0).astype(jnp.bfloat16)
    span_out = jnp.einsum('qhk,khd->qhd', weights.astype(jnp.float32), value_block)
    return (span_out, lax.optimization_barrier(jnp.sum(failure, axis=2)))

def attend(queries, keys, values, key_bias):
    span_count = SEQUENCE_LENGTH // SPAN
    query_spans = queries.astype(jnp.float32).reshape(span_count, SPAN, HEAD_COUNT, HEAD_DIM)
    key_spans = keys.astype(jnp.float32).reshape(span_count, SPAN, HEAD_COUNT, HEAD_DIM)
    value_spans = values.astype(jnp.float32).reshape(span_count, SPAN, HEAD_COUNT, HEAD_DIM)
    bias_spans = key_bias.astype(jnp.float32).reshape(span_count, SPAN, HEAD_COUNT)

    def per_block(inputs):
        query_block, block_index = inputs
        query_pos = block_index * SPAN + jnp.arange(SPAN, dtype=jnp.int32)

        def step(held, key_index):
            running, after_total = held

            def compute():
                key_pos = key_index * SPAN + jnp.arange(SPAN, dtype=jnp.int32)
                return stick_span(query_block, key_spans[key_index], value_spans[key_index], bias_spans[key_index], query_pos, key_pos)

            def skipped():
                return (jnp.zeros((SPAN, HEAD_COUNT, HEAD_DIM), jnp.float32), jnp.zeros((SPAN, HEAD_COUNT), jnp.float32))
            span_out, span_sum = lax.cond(key_index <= block_index, compute, skipped)
            return ((running + jnp.exp(after_total)[..., None] * span_out, after_total + span_sum), None)
        start_pair = (jnp.zeros((SPAN, HEAD_COUNT, HEAD_DIM), jnp.float32), jnp.zeros((SPAN, HEAD_COUNT), jnp.float32))
        (running, _), _ = lax.scan(step, start_pair, jnp.arange(span_count, dtype=jnp.int32), reverse=True)
        return running.astype(jnp.bfloat16)
    blocks = lax.map(per_block, (query_spans, jnp.arange(span_count, dtype=jnp.int32)))
    return blocks.reshape(SEQUENCE_LENGTH, HEAD_COUNT * HEAD_DIM)

def experts_out(normed, routes, route_weights, gate_weight, up_weight, down_weight):
    most_rows = SEQUENCE_LENGTH // TOK_DEV * CAP
    flat_routes = routes.reshape(-1)
    flat_weights = route_weights.reshape(-1)
    token_of = (jnp.arange(SEQUENCE_LENGTH * TOP, dtype=jnp.int32) // TOP).astype(jnp.int32)
    block_units = FF // N_TP

    def one_expert(total, expert_index):
        chosen = flat_routes == expert_index
        picked = jnp.nonzero(chosen, size=most_rows, fill_value=0)[0].astype(jnp.int32)
        row_valid = jnp.arange(most_rows, dtype=jnp.int32) < jnp.sum(chosen.astype(jnp.int32))
        token_ids = token_of[picked]
        row_block = normed[token_ids]
        gate_act = jnp.dot(row_block, gate_weight[expert_index], preferred_element_type=jnp.float32)
        up_act = jnp.dot(row_block, up_weight[expert_index], preferred_element_type=jnp.float32)
        hidden = (jax.nn.silu(gate_act) * up_act).astype(jnp.bfloat16)
        summed = jnp.zeros((most_rows, D), jnp.float32)
        for block in range(N_TP):
            lower = block * block_units
            partial_value = jnp.dot(hidden[:, lower:lower + block_units], down_weight[expert_index, lower:lower + block_units], preferred_element_type=jnp.float32)
            summed = summed + lax.optimization_barrier(partial_value.astype(jnp.bfloat16)).astype(jnp.float32)
        expert_rows = lax.optimization_barrier(summed.astype(jnp.bfloat16)).astype(jnp.float32)
        scaled = jnp.where(row_valid[:, None], flat_weights[picked][:, None] * expert_rows, 0.0)
        return (total.at[token_ids].add(scaled), None)
    routed, _ = lax.scan(one_expert, jnp.zeros((SEQUENCE_LENGTH, D), jnp.float32), jnp.arange(EXPERTS, dtype=jnp.int32))
    return routed

def reference(queries, keys, values, key_bias, residual, out_weight, norm_gain, routes, route_weights, gate_weight, up_weight, down_weight):
    attended = attend(queries, keys, values, key_bias)
    mixed_rows = (residual.astype(jnp.float32) + jnp.dot(attended, out_weight, preferred_element_type=jnp.float32)).astype(jnp.bfloat16)
    stream = mixed_rows.astype(jnp.float32)
    normed = (stream * lax.rsqrt(lax.optimization_barrier(jnp.mean(stream * stream, axis=-1, keepdims=True)) + epsilon) * norm_gain).astype(jnp.bfloat16)
    routed = experts_out(normed, routes, route_weights, gate_weight, up_weight, down_weight)
    return (stream + routed).astype(jnp.bfloat16)
```

```python
import functools

import jax
import jax.numpy as jnp
from jax import lax
from jax.experimental import pallas as pl
from jax.experimental.pallas import tpu as pltpu
from jax.sharding import PartitionSpec as P

HEAD_DIM = 64
TOP = 2
SPAN = 512
BLOCK = 256
QUERY_ROWS = 256
BIAS_ROWS = 16
MESH = pl.DeviceIdType.MESH


epsilon = 1e-06


def attend_kernel(
    n, length, heads, q_ref, own_ref, out_ref, held, total, after, tri, up_sem, side_sem, recv_sem
):
    me = lax.axis_index("sp")
    odd = lax.rem(me, 2)
    partner = me + 1 - 2 * odd
    has_up = me + 2 < n
    has_down = me >= 2
    barrier = pltpu.get_barrier_semaphore()

    def greet(device):
        pl.semaphore_signal(barrier, inc=1, device_id={"sp": device}, device_id_type=MESH)

    greet(partner)
    pl.when(has_up)(lambda: greet(me + 2))
    pl.when(has_down)(lambda: greet(me - 2))

    total[...] = jnp.zeros_like(total)
    after[...] = jnp.zeros_like(after)
    tri_row = lax.broadcasted_iota(jnp.int32, (BLOCK, BLOCK), 0)
    tri_col = lax.broadcasted_iota(jnp.int32, (BLOCK, BLOCK), 1)
    tri[...] = (tri_row > tri_col).astype(jnp.float32).astype(jnp.bfloat16)

    pl.semaphore_wait(barrier, 1 + has_up.astype(jnp.int32) + has_down.astype(jnp.int32))

    def up(d, source):
        return pltpu.make_async_remote_copy(
            src_ref=source,
            dst_ref=held.at[d + 2],
            send_sem=up_sem.at[d],
            recv_sem=recv_sem.at[d + 2],
            device_id={"sp": me + 2},
            device_id_type=MESH,
        )

    def side(d, slot, source):
        return pltpu.make_async_remote_copy(
            src_ref=source,
            dst_ref=held.at[slot],
            send_sem=side_sem.at[d],
            recv_sem=recv_sem.at[slot],
            device_id={"sp": partner},
            device_id_type=MESH,
        )

    def send(d, source):
        pl.when(has_up)(lambda: up(d, source).start())
        pl.when(odd == 0)(lambda: side(d, d + 1, source).start())
        pl.when((odd == 1) & (d >= 2))(lambda: side(d, d - 1, source).start())

    width = heads * HEAD_DIM
    row_width = 2 * width
    lane = lax.broadcasted_iota(jnp.int32, (QUERY_ROWS, width), 1)
    tile_blocks = SPAN // BLOCK

    def bias_row(bias_rows, h, start):
        step = min(row_width, BLOCK)
        pieces = []
        for first in range(0, BLOCK, step):
            flat = h * length + start + first
            row, col = flat // row_width, flat % row_width
            pieces.append(bias_rows[row : row + 1, col : col + step])
        return jnp.concatenate(pieces, axis=1) if len(pieces) > 1 else pieces[0]

    def tile(source, span, q0, masked):
        k0 = span * SPAN
        key_rows = source[k0 : k0 + SPAN, :width]
        value_rows = source[k0 : k0 + SPAN, width:row_width]
        bias_rows = source[length : length + BIAS_ROWS, :].astype(jnp.float32)
        gathered = None
        for h in range(heads):
            query = q_ref[h, pl.ds(q0, QUERY_ROWS), :]
            later = jnp.zeros((QUERY_ROWS, 1), jnp.float32)
            weights = [None] * tile_blocks
            for block in reversed(range(tile_blocks)):
                b0 = block * BLOCK
                scores = lax.dot_general(
                    query,
                    key_rows[b0 : b0 + BLOCK],
                    (((1,), (1,)), ((), ())),
                    preferred_element_type=jnp.float32,
                )
                scores = scores + bias_row(bias_rows, h, k0 + b0)
                soft = jnp.maximum(scores, 0.0) + jnp.log(1.0 + jnp.exp(-jnp.abs(scores)))
                rest = scores - soft
                if masked:
                    q_pos = q0 - k0 + lax.broadcasted_iota(jnp.int32, scores.shape, 0)
                    k_pos = b0 + lax.broadcasted_iota(jnp.int32, scores.shape, 1)
                    earlier = k_pos < q_pos
                    soft = jnp.where(earlier, soft, 0.0)
                high = soft.astype(jnp.bfloat16)
                low = (soft - high.astype(jnp.float32)).astype(jnp.bfloat16)
                beyond = jnp.dot(high, tri[...], preferred_element_type=jnp.float32) + jnp.dot(
                    low, tri[...], preferred_element_type=jnp.float32
                )
                beyond = beyond + later
                piece = jnp.exp(rest - beyond)
                if masked:
                    piece = jnp.where(earlier, piece, 0.0)
                weights[block] = piece.astype(jnp.bfloat16)
                later = beyond[:, :1] + soft[:, :1]
            joined = jnp.concatenate(weights, axis=1)
            span_out = jnp.dot(joined, value_rows, preferred_element_type=jnp.float32)
            rows = pl.ds(q0, QUERY_ROWS)
            held_after = after[h, rows, :]
            span_out = jnp.exp(-held_after[:, :width]) * span_out
            after[h, rows, :] = held_after + later
            if gathered is None:
                gathered = span_out
            else:
                gathered = jnp.where(lane >= h * HEAD_DIM, span_out, gathered)
        rows = pl.ds(q0, QUERY_ROWS)
        total[rows, :] = total[rows, :] + gathered

    span_count = length // SPAN

    def compute(source, own):
        def chunk(c, carry):
            q0 = pl.multiple_of(c * QUERY_ROWS, QUERY_ROWS)
            for span in reversed(range(span_count)):
                if own:
                    span_of = q0 // SPAN
                    pl.when(span_of == span)(lambda: tile(source, span, q0, True))
                    if span < span_count - 1:
                        pl.when(span_of > span)(lambda: tile(source, span, q0, False))
                else:
                    tile(source, span, q0, False)
            return carry

        lax.fori_loop(0, length // QUERY_ROWS, chunk, 0)

    send(0, own_ref)
    compute(own_ref, True)

    def arrive(d, carry):
        pltpu.make_async_remote_copy(
            src_ref=held.at[d],
            dst_ref=held.at[d],
            send_sem=up_sem.at[d],
            recv_sem=recv_sem.at[d],
            device_id={"sp": partner},
            device_id_type=MESH,
        ).wait_recv()
        pl.when(lax.rem(d, 2) == 0)(lambda: send(d, held.at[d]))
        compute(held.at[d], False)
        return carry

    lax.fori_loop(1, me + 1, arrive, 0)
    out_ref[...] = total[...].astype(jnp.bfloat16)

    def sent(d, source):
        pl.when(has_up)(lambda: up(d, source).wait_send())
        pl.when(odd == 0)(lambda: side(d, d + 1, source).wait_send())
        pl.when((odd == 1) & (d >= 2))(lambda: side(d, d - 1, source).wait_send())

    sent(0, own_ref)

    def drain(half, carry):
        sent(2 * half, held.at[2 * half])
        return carry

    lax.fori_loop(1, me // 2 + 1, drain, 0)


def attend(queries, keys, values, key_bias):
    n = lax.axis_size("sp")
    length = queries.shape[0]
    heads = key_bias.shape[1]
    width = heads * HEAD_DIM
    row_width = 2 * width
    head_of = lax.iota(jnp.int32, width) // HEAD_DIM
    scaled = queries * jnp.bfloat16(HEAD_DIM ** (-0.5))
    per_head = jnp.where(
        head_of[None, None, :] == lax.iota(jnp.int32, heads)[:, None, None],
        scaled[None],
        jnp.bfloat16(0),
    )
    bias_rows = jnp.transpose(key_bias).reshape(-1, row_width)
    bias_rows = jnp.pad(bias_rows, ((0, BIAS_ROWS - bias_rows.shape[0]), (0, 0)))
    own = jnp.concatenate([jnp.concatenate([keys, values], axis=1), bias_rows], axis=0)
    vmem = pl.BlockSpec(memory_space=pltpu.VMEM)
    return pl.pallas_call(
        functools.partial(attend_kernel, n, length, heads),
        out_shape=jax.ShapeDtypeStruct((length, width), jnp.bfloat16),
        in_specs=[vmem, vmem],
        out_specs=vmem,
        scratch_shapes=[
            pltpu.VMEM((n, length + BIAS_ROWS, row_width), jnp.bfloat16),
            pltpu.VMEM((length, width), jnp.float32),
            pltpu.VMEM((heads, length, 128), jnp.float32),
            pltpu.VMEM((BLOCK, BLOCK), jnp.bfloat16),
            pltpu.SemaphoreType.DMA((n + 2,)),
            pltpu.SemaphoreType.DMA((n + 2,)),
            pltpu.SemaphoreType.DMA((n + 2,)),
        ],
        compiler_params=pltpu.CompilerParams(
            collective_id=0, has_side_effects=True, vmem_limit_bytes=40 * 1024 * 1024
        ),
        name="attend",
    )(per_head, own)


def shards(
    queries,
    keys,
    values,
    key_bias,
    residual,
    out_weight,
    norm_gain,
    routes,
    route_weights,
    gate_weight,
    up_weight,
    down_weight,
):
    sp_count = lax.axis_size("sp")
    attended = attend(queries, keys, values, key_bias)
    token_heads = lax.all_to_all(attended, "tp", split_axis=0, concat_axis=1, tiled=True)
    projected = jnp.dot(token_heads, out_weight, preferred_element_type=jnp.float32)
    stream = (residual.astype(jnp.float32) + projected).astype(jnp.bfloat16).astype(jnp.float32)
    normed = (
        stream * lax.rsqrt(jnp.mean(stream * stream, axis=-1, keepdims=True) + epsilon) * norm_gain
    ).astype(jnp.bfloat16)
    token_count = residual.shape[0]
    width_model = residual.shape[1]
    capacity = max(2, 5 * token_count * TOP // (4 * sp_count))
    flat_routes = routes.reshape(-1)
    onehot = (flat_routes[:, None] == lax.iota(jnp.int32, sp_count)[None, :]).astype(jnp.int32)
    before = jnp.cumsum(onehot, axis=0) - onehot
    slot_of = flat_routes * capacity + jnp.sum(before * onehot, axis=1)
    select = (slot_of[:, None] == lax.iota(jnp.int32, sp_count * capacity)[None, :]).astype(
        jnp.bfloat16
    )
    placing = jnp.sum(select.reshape(token_count, TOP, sp_count * capacity), axis=1)
    outgoing = jnp.einsum("ts,td->sd", placing, normed, preferred_element_type=jnp.float32).astype(
        jnp.bfloat16
    )
    arrived = lax.all_to_all(outgoing, "sp", split_axis=0, concat_axis=0, tiled=True)
    row_block = lax.all_gather(arrived, "tp", axis=0, tiled=True)
    gate_act = jnp.dot(row_block, gate_weight[0], preferred_element_type=jnp.float32)
    up_act = jnp.dot(row_block, up_weight[0], preferred_element_type=jnp.float32)
    hidden = (jax.nn.silu(gate_act) * up_act).astype(jnp.bfloat16)
    partial_value = jnp.dot(hidden, down_weight[0], preferred_element_type=jnp.float32)
    summed = lax.psum_scatter(
        lax.optimization_barrier(partial_value.astype(jnp.bfloat16))
        .astype(jnp.float32)
        .astype(jnp.bfloat16),
        "tp",
        scatter_dimension=0,
        tiled=True,
    )
    returned = lax.all_to_all(summed, "sp", split_axis=0, concat_axis=0, tiled=True)
    picked = jnp.dot(select, returned, preferred_element_type=jnp.float32).reshape(
        token_count, TOP, width_model
    )
    routed = jnp.sum(picked * route_weights[:, :, None], axis=1)
    return (stream + routed).astype(jnp.bfloat16)


def solution(mesh):
    return jax.shard_map(
        shards,
        mesh=mesh,
        in_specs=(
            P("sp", "tp"),
            P("sp", "tp"),
            P("sp", "tp"),
            P("sp", "tp"),
            P(("sp", "tp"), None),
            P(),
            P(),
            P(("sp", "tp"), None),
            P(("sp", "tp"), None),
            P("sp", None, "tp"),
            P("sp", None, "tp"),
            P("sp", "tp", None),
        ),
        out_specs=P(("sp", "tp"), None),
        check_vma=False,
    )
```

```python
import functools

import jax
import jax.numpy as jnp
from jax import lax
from jax.experimental import pallas as pl
from jax.experimental.pallas import tpu as pltpu
from jax.sharding import PartitionSpec as P

HEAD_DIM = 64
TOP = 2
SPAN = 512
BLOCK = 256
QUERY_ROWS = 256
BIAS_ROWS = 16
MESH = pl.DeviceIdType.MESH


epsilon = 1e-06


def attend_kernel(
    n, length, heads, q_ref, own_ref, out_ref, held, total, after, tri, up_sem, side_sem, recv_sem
):
    me = lax.axis_index("sp")
    odd = lax.rem(me, 2)
    partner = me + 1 - 2 * odd
    has_up = me + 2 < n
    has_down = me >= 2
    barrier = pltpu.get_barrier_semaphore()

    def greet(device):
        pl.semaphore_signal(barrier, inc=1, device_id={"sp": device}, device_id_type=MESH)

    greet(partner)
    pl.when(has_up)(lambda: greet(me + 2))
    pl.when(has_down)(lambda: greet(me - 2))

    total[...] = jnp.zeros_like(total)
    after[...] = jnp.zeros_like(after)
    tri_row = lax.broadcasted_iota(jnp.int32, (BLOCK, BLOCK), 0)
    tri_col = lax.broadcasted_iota(jnp.int32, (BLOCK, BLOCK), 1)
    tri[...] = (tri_row > tri_col).astype(jnp.float32).astype(jnp.bfloat16)

    pl.semaphore_wait(barrier, 1 + has_up.astype(jnp.int32) + has_down.astype(jnp.int32))

    def up(d, source):
        return pltpu.make_async_remote_copy(
            src_ref=source,
            dst_ref=held.at[d + 2],
            send_sem=up_sem.at[d],
            recv_sem=recv_sem.at[d + 2],
            device_id={"sp": me + 2},
            device_id_type=MESH,
        )

    def side(d, slot, source):
        return pltpu.make_async_remote_copy(
            src_ref=source,
            dst_ref=held.at[slot],
            send_sem=side_sem.at[d],
            recv_sem=recv_sem.at[slot],
            device_id={"sp": partner},
            device_id_type=MESH,
        )

    def send(d, source):
        pl.when(has_up)(lambda: up(d, source).start())
        pl.when(odd == 0)(lambda: side(d, d + 1, source).start())
        pl.when((odd == 1) & (d >= 2))(lambda: side(d, d - 1, source).start())

    width = heads * HEAD_DIM
    row_width = 2 * width
    lane = lax.broadcasted_iota(jnp.int32, (QUERY_ROWS, width), 1)
    tile_blocks = SPAN // BLOCK

    def bias_row(bias_rows, h, start):
        step = min(row_width, BLOCK)
        pieces = []
        for first in range(0, BLOCK, step):
            flat = h * length + start + first
            row, col = flat // row_width, flat % row_width
            pieces.append(bias_rows[row : row + 1, col : col + step])
        return jnp.concatenate(pieces, axis=1) if len(pieces) > 1 else pieces[0]

    def tile(source, span, q0, masked):
        k0 = span * SPAN
        key_rows = source[k0 : k0 + SPAN, :width]
        value_rows = source[k0 : k0 + SPAN, width:row_width]
        bias_rows = source[length : length + BIAS_ROWS, :].astype(jnp.float32)
        gathered = None
        for h in range(heads):
            query = q_ref[h, pl.ds(q0, QUERY_ROWS), :]
            later = jnp.zeros((QUERY_ROWS, 1), jnp.float32)
            weights = [None] * tile_blocks
            for block in reversed(range(tile_blocks)):
                b0 = block * BLOCK
                scores = lax.dot_general(
                    query,
                    key_rows[b0 : b0 + BLOCK],
                    (((1,), (1,)), ((), ())),
                    preferred_element_type=jnp.float32,
                )
                scores = scores + bias_row(bias_rows, h, k0 + b0)
                soft = jnp.maximum(scores, 0.0) + jnp.log(1.0 + jnp.exp(-jnp.abs(scores)))
                rest = scores - soft
                if masked:
                    q_pos = q0 - k0 + lax.broadcasted_iota(jnp.int32, scores.shape, 0)
                    k_pos = b0 + lax.broadcasted_iota(jnp.int32, scores.shape, 1)
                    earlier = k_pos < q_pos
                    soft = jnp.where(earlier, soft, 0.0)
                high = soft.astype(jnp.bfloat16)
                low = (soft - high.astype(jnp.float32)).astype(jnp.bfloat16)
                beyond = jnp.dot(high, tri[...], preferred_element_type=jnp.float32) + jnp.dot(
                    low, tri[...], preferred_element_type=jnp.float32
                )
                beyond = beyond + later
                piece = jnp.exp(rest - beyond)
                if masked:
                    piece = jnp.where(earlier, piece, 0.0)
                weights[block] = piece.astype(jnp.bfloat16)
                later = beyond[:, :1] + soft[:, :1]
            joined = jnp.concatenate(weights, axis=1)
            span_out = jnp.dot(joined, value_rows, preferred_element_type=jnp.float32)
            rows = pl.ds(q0, QUERY_ROWS)
            held_after = after[h, rows, :]
            span_out = jnp.exp(-held_after[:, :width]) * span_out
            after[h, rows, :] = held_after + later
            if gathered is None:
                gathered = span_out
            else:
                gathered = jnp.where(lane >= h * HEAD_DIM, span_out, gathered)
        rows = pl.ds(q0, QUERY_ROWS)
        total[rows, :] = total[rows, :] + gathered

    span_count = length // SPAN

    def compute(source, own):
        def chunk(c, carry):
            q0 = pl.multiple_of(c * QUERY_ROWS, QUERY_ROWS)
            for span in reversed(range(span_count)):
                if own:
                    span_of = q0 // SPAN
                    pl.when(span_of == span)(lambda: tile(source, span, q0, True))
                    if span < span_count - 1:
                        pl.when(span_of > span)(lambda: tile(source, span, q0, False))
                else:
                    tile(source, span, q0, False)
            return carry

        lax.fori_loop(0, length // QUERY_ROWS, chunk, 0)

    send(0, own_ref)
    compute(own_ref, True)

    def arrive(d, carry):
        pltpu.make_async_remote_copy(
            src_ref=held.at[d],
            dst_ref=held.at[d],
            send_sem=up_sem.at[d],
            recv_sem=recv_sem.at[d],
            device_id={"sp": partner},
            device_id_type=MESH,
        ).wait_recv()
        pl.when(lax.rem(d, 2) == 0)(lambda: send(d, held.at[d]))
        compute(held.at[d], False)
        return carry

    lax.fori_loop(1, me + 1, arrive, 0)
    out_ref[...] = total[...].astype(jnp.bfloat16)

    def sent(d, source):
        pl.when(has_up)(lambda: up(d, source).wait_send())
        pl.when(odd == 0)(lambda: side(d, d + 1, source).wait_send())
        pl.when((odd == 1) & (d >= 2))(lambda: side(d, d - 1, source).wait_send())

    sent(0, own_ref)

    def drain(half, carry):
        sent(2 * half, held.at[2 * half])
        return carry

    lax.fori_loop(1, me // 2 + 1, drain, 0)


def attend(queries, keys, values, key_bias):
    n = lax.axis_size("sp")
    length = queries.shape[0]
    heads = key_bias.shape[1]
    width = heads * HEAD_DIM
    row_width = 2 * width
    head_of = lax.iota(jnp.int32, width) // HEAD_DIM
    scaled = queries * jnp.bfloat16(HEAD_DIM ** (-0.5))
    per_head = jnp.where(
        head_of[None, None, :] == lax.iota(jnp.int32, heads)[:, None, None],
        scaled[None],
        jnp.bfloat16(0),
    )
    bias_rows = jnp.transpose(key_bias).reshape(-1, row_width)
    bias_rows = jnp.pad(bias_rows, ((0, BIAS_ROWS - bias_rows.shape[0]), (0, 0)))
    own = jnp.concatenate([jnp.concatenate([keys, values], axis=1), bias_rows], axis=0)
    vmem = pl.BlockSpec(memory_space=pltpu.VMEM)
    return pl.pallas_call(
        functools.partial(attend_kernel, n, length, heads),
        out_shape=jax.ShapeDtypeStruct((length, width), jnp.bfloat16),
        in_specs=[vmem, vmem],
        out_specs=vmem,
        scratch_shapes=[
            pltpu.VMEM((n, length + BIAS_ROWS, row_width), jnp.bfloat16),
            pltpu.VMEM((length, width), jnp.float32),
            pltpu.VMEM((heads, length, 128), jnp.float32),
            pltpu.VMEM((BLOCK, BLOCK), jnp.bfloat16),
            pltpu.SemaphoreType.DMA((n + 2,)),
            pltpu.SemaphoreType.DMA((n + 2,)),
            pltpu.SemaphoreType.DMA((n + 2,)),
        ],
        compiler_params=pltpu.CompilerParams(
            collective_id=0, has_side_effects=True, vmem_limit_bytes=40 * 1024 * 1024
        ),
        name="attend",
    )(per_head, own)


def dispatch_kernel(n, groups, outgoing, rows, sp_sem, chip_sem, core_sem, recv_sem):
    me, my_t = lax.axis_index("sp"), lax.axis_index("tp")
    mate = my_t + 1 - 2 * lax.rem(my_t, 2)
    chips = groups // 2
    alike = [lax.rem(my_t + 2 * k, groups) for k in range(1, chips)]
    greet_all(n, me, mate, alike)

    def copy(source, t, s, send_sem, device):
        return pltpu.make_async_remote_copy(
            src_ref=source,
            dst_ref=rows.at[t * n + s],
            send_sem=send_sem,
            recv_sem=recv_sem.at[t * n + s],
            device_id=device,
            device_id_type=MESH,
        )

    def to_expert(r):
        target = lax.rem(me + r, n)
        return copy(outgoing.at[target], my_t, me, sp_sem.at[r], {"sp": target})

    def to_chip(k, s, source):
        return copy(source, my_t, s, chip_sem.at[k * n + s], {"tp": alike[k]})

    def to_mate(t, s, source):
        return copy(source, t, s, core_sem.at[t * n + s], {"tp": mate})

    def arrived(t, s):
        copy(rows.at[t * n + s], t, s, core_sem.at[t * n + s], {"tp": mate}).wait_recv()

    def spread(s, source):
        for k in range(chips - 1):
            to_chip(k, s, source).start()
        to_mate(my_t, s, source).start()

    def relay(r):
        s = lax.rem(me + n - r, n)
        for t in alike:
            arrived(t, s)
            to_mate(t, s, rows.at[t * n + s]).start()

    def issue(r, carry):
        to_expert(r).start()
        return carry

    spread(me, outgoing.at[me])
    lax.fori_loop(1, n, issue, 0)
    rows[my_t * n + me] = outgoing[me]

    def step(r, carry):
        s = lax.rem(me + n - r, n)
        arrived(my_t, s)
        spread(s, rows.at[my_t * n + s])
        relay(r - 1)
        return carry

    lax.fori_loop(1, n, step, 0)
    relay(n - 1)

    def finish(s, carry):
        arrived(mate, s)
        for t in alike:
            arrived(t + 1 - 2 * lax.rem(t, 2), s)
        pl.when(s >= 1)(lambda: to_expert(s).wait_send())
        for k in range(chips - 1):
            to_chip(k, s, outgoing.at[me]).wait_send()
            to_mate(alike[k], s, outgoing.at[me]).wait_send()
        to_mate(my_t, s, outgoing.at[me]).wait_send()
        return carry

    lax.fori_loop(0, n, finish, 0)


def greet_all(n, me, mate, alike):
    barrier = pltpu.get_barrier_semaphore()

    def greet(device):
        pl.semaphore_signal(barrier, inc=1, device_id=device, device_id_type=MESH)

    def greet_sp(r, carry):
        greet({"sp": lax.rem(me + r, n)})
        return carry

    lax.fori_loop(1, n, greet_sp, 0)
    greet({"tp": mate})
    for t in alike:
        greet({"tp": t})
    pl.semaphore_wait(barrier, n + len(alike))


def combine_kernel(
    n, groups, partial, back, pair, other, done, pair_send, pair_recv, chip_send, chip_recv,
    back_send, back_recv,
):
    me, my_t = lax.axis_index("sp"), lax.axis_index("tp")
    core = lax.rem(my_t, 2)
    mate = my_t + 1 - 2 * core
    chips = groups // 2
    alike = [lax.rem(my_t + 2 * k, groups) for k in range(1, chips)]
    greet_all(n, me, mate, alike)

    def home(r):
        return lax.rem(me + 1 + r, n)

    def pair_copy(chip, r):
        return pltpu.make_async_remote_copy(
            src_ref=partial.at[(2 * chip + 1 - core) * n + home(r)],
            dst_ref=pair.at[chip * n + r],
            send_sem=pair_send.at[chip * n + r],
            recv_sem=pair_recv.at[chip * n + r],
            device_id={"tp": mate},
            device_id_type=MESH,
        )

    def chip_copy(k, r):
        return pltpu.make_async_remote_copy(
            src_ref=pair.at[(alike[k] // 2) * n + r],
            dst_ref=other.at[k * n + r],
            send_sem=chip_send.at[k * n + r],
            recv_sem=chip_recv.at[k * n + r],
            device_id={"tp": alike[k]},
            device_id_type=MESH,
        )

    def back_copy(r):
        return pltpu.make_async_remote_copy(
            src_ref=done.at[r],
            dst_ref=back.at[me],
            send_sem=back_send.at[r],
            recv_sem=back_recv.at[me],
            device_id={"sp": home(r)},
            device_id_type=MESH,
        )

    def start_pairs(r, carry):
        for chip in range(chips):
            pair_copy(chip, r).start()
        return carry

    lax.fori_loop(0, n, start_pairs, 0)

    def add_pairs(r):
        for chip in range(chips):
            pair_copy(chip, r).wait_recv()
        for k in range(chips - 1):
            chip = alike[k] // 2
            pair[chip * n + r] = (
                partial[alike[k] * n + home(r)].astype(jnp.float32)
                + pair[chip * n + r].astype(jnp.float32)
            ).astype(jnp.bfloat16)

    def add_chips(r):
        value = partial[my_t * n + home(r)].astype(jnp.float32) + pair[
            (my_t // 2) * n + r
        ].astype(jnp.float32)
        for k in range(chips - 1):
            chip_copy(k, r).wait_recv()
            value = value + other[k * n + r].astype(jnp.float32)
        return value.astype(jnp.bfloat16)

    def send_chips(r):
        for k in range(chips - 1):
            chip_copy(k, r).start()

    lag = 1
    for r in range(lag):
        add_pairs(r)
        send_chips(r)

    def step(r, carry):
        add_pairs(r)
        send_chips(r)
        done[r - lag] = add_chips(r - lag)
        back_copy(r - lag).start()
        return carry

    lax.fori_loop(lag, n, step, 0)
    for r in range(n - lag, n):
        if r == n - 1:
            back[me] = add_chips(r)
        else:
            done[r] = add_chips(r)
            back_copy(r).start()

    def finish(r, carry):
        for chip in range(chips):
            pair_copy(chip, r).wait_send()
        for k in range(chips - 1):
            chip_copy(k, r).wait_send()
        return carry

    lax.fori_loop(0, n, finish, 0)

    def finish_back(r, carry):
        back_copy(r).wait_send()
        source = home(r)
        pltpu.make_async_remote_copy(
            src_ref=done.at[r],
            dst_ref=back.at[source],
            send_sem=back_send.at[r],
            recv_sem=back_recv.at[source],
            device_id={"sp": source},
            device_id_type=MESH,
        ).wait_recv()
        return carry

    lax.fori_loop(0, n - 1, finish_back, 0)


def dispatch(outgoing):
    n, groups = lax.axis_size("sp"), lax.axis_size("tp")
    chips = groups // 2
    _, capacity, width = outgoing.shape
    vmem = pl.BlockSpec(memory_space=pltpu.VMEM)
    return pl.pallas_call(
        functools.partial(dispatch_kernel, n, groups),
        out_shape=jax.ShapeDtypeStruct((groups * n, capacity, width), outgoing.dtype),
        in_specs=[vmem],
        out_specs=vmem,
        scratch_shapes=[
            pltpu.SemaphoreType.DMA((n,)),
            pltpu.SemaphoreType.DMA((max(1, chips - 1) * n,)),
            pltpu.SemaphoreType.DMA((groups * n,)),
            pltpu.SemaphoreType.DMA((groups * n,)),
        ],
        compiler_params=pltpu.CompilerParams(
            collective_id=1, has_side_effects=True, vmem_limit_bytes=56 * 1024 * 1024
        ),
        name="dispatch",
    )(outgoing)


def combine(partial):
    n, groups = lax.axis_size("sp"), lax.axis_size("tp")
    chips = groups // 2
    _, capacity, width = partial.shape
    vmem = pl.BlockSpec(memory_space=pltpu.VMEM)
    apart = max(1, chips - 1) * n
    return pl.pallas_call(
        functools.partial(combine_kernel, n, groups),
        out_shape=jax.ShapeDtypeStruct((n, capacity, width), partial.dtype),
        in_specs=[vmem],
        out_specs=vmem,
        scratch_shapes=[
            pltpu.VMEM((chips * n, capacity, width), partial.dtype),
            pltpu.VMEM((apart, capacity, width), partial.dtype),
            pltpu.VMEM((n, capacity, width), partial.dtype),
            pltpu.SemaphoreType.DMA((chips * n,)),
            pltpu.SemaphoreType.DMA((chips * n,)),
            pltpu.SemaphoreType.DMA((apart,)),
            pltpu.SemaphoreType.DMA((apart,)),
            pltpu.SemaphoreType.DMA((n,)),
            pltpu.SemaphoreType.DMA((n,)),
        ],
        compiler_params=pltpu.CompilerParams(
            collective_id=2, has_side_effects=True, vmem_limit_bytes=56 * 1024 * 1024
        ),
        name="combine",
    )(partial)


def shards(
    queries,
    keys,
    values,
    key_bias,
    residual,
    out_weight,
    norm_gain,
    routes,
    route_weights,
    gate_weight,
    up_weight,
    down_weight,
):
    sp_count = lax.axis_size("sp")
    attended = attend(queries, keys, values, key_bias)
    token_heads = lax.all_to_all(attended, "tp", split_axis=0, concat_axis=1, tiled=True)
    projected = jnp.dot(token_heads, out_weight, preferred_element_type=jnp.float32)
    stream = (residual.astype(jnp.float32) + projected).astype(jnp.bfloat16).astype(jnp.float32)
    normed = (
        stream * lax.rsqrt(jnp.mean(stream * stream, axis=-1, keepdims=True) + epsilon) * norm_gain
    ).astype(jnp.bfloat16)
    token_count = residual.shape[0]
    width_model = residual.shape[1]
    capacity = max(2, 5 * token_count * TOP // (4 * sp_count))
    flat_routes = routes.reshape(-1)
    onehot = (flat_routes[:, None] == lax.iota(jnp.int32, sp_count)[None, :]).astype(jnp.int32)
    before = jnp.cumsum(onehot, axis=0) - onehot
    slot_of = flat_routes * capacity + jnp.sum(before * onehot, axis=1)
    select = (slot_of[:, None] == lax.iota(jnp.int32, sp_count * capacity)[None, :]).astype(
        jnp.bfloat16
    )
    placing = jnp.sum(select.reshape(token_count, TOP, sp_count * capacity), axis=1)
    outgoing = jnp.einsum("ts,td->sd", placing, normed, preferred_element_type=jnp.float32).astype(
        jnp.bfloat16
    )
    row_block = dispatch(outgoing.reshape(sp_count, capacity, width_model)).reshape(-1, width_model)
    gate_act = jnp.dot(row_block, gate_weight[0], preferred_element_type=jnp.float32)
    up_act = jnp.dot(row_block, up_weight[0], preferred_element_type=jnp.float32)
    hidden = (jax.nn.silu(gate_act) * up_act).astype(jnp.bfloat16)
    partial_value = jnp.dot(hidden, down_weight[0], preferred_element_type=jnp.float32)
    returned = combine(
        partial_value.astype(jnp.bfloat16).reshape(-1, capacity, width_model)
    ).reshape(-1, width_model)
    picked = jnp.dot(select, returned, preferred_element_type=jnp.float32).reshape(
        token_count, TOP, width_model
    )
    routed = jnp.sum(picked * route_weights[:, :, None], axis=1)
    return (stream + routed).astype(jnp.bfloat16)


def solution(mesh):
    return jax.shard_map(
        shards,
        mesh=mesh,
        in_specs=(
            P("sp", "tp"),
            P("sp", "tp"),
            P("sp", "tp"),
            P("sp", "tp"),
            P(("sp", "tp"), None),
            P(),
            P(),
            P(("sp", "tp"), None),
            P(("sp", "tp"), None),
            P("sp", None, "tp"),
            P("sp", None, "tp"),
            P("sp", "tp", None),
        ),
        out_specs=P(("sp", "tp"), None),
        check_vma=False,
    )
```

```python
import functools

import jax
import jax.numpy as jnp
from jax import lax
from jax.experimental import pallas as pl
from jax.experimental.pallas import tpu as pltpu
from jax.sharding import PartitionSpec as P

HEAD_DIM = 64
TOP = 2
SPAN = 512
BLOCK = 256
QUERY_ROWS = 256
BIAS_ROWS = 16
MESH = pl.DeviceIdType.MESH


epsilon = 1e-06


def attend_kernel(
    n, length, heads, q_ref, own_ref, out_ref, held, total, after, tri, up_sem, side_sem, recv_sem
):
    me = lax.axis_index("sp")
    odd = lax.rem(me, 2)
    partner = me + 1 - 2 * odd
    has_up = me + 2 < n
    has_down = me >= 2
    barrier = pltpu.get_barrier_semaphore()

    def greet(device):
        pl.semaphore_signal(barrier, inc=1, device_id={"sp": device}, device_id_type=MESH)

    greet(partner)
    pl.when(has_up)(lambda: greet(me + 2))
    pl.when(has_down)(lambda: greet(me - 2))

    total[...] = jnp.zeros_like(total)
    after[...] = jnp.zeros_like(after)
    tri_row = lax.broadcasted_iota(jnp.int32, (BLOCK, BLOCK), 0)
    tri_col = lax.broadcasted_iota(jnp.int32, (BLOCK, BLOCK), 1)
    tri[...] = (tri_row > tri_col).astype(jnp.float32).astype(jnp.bfloat16)

    pl.semaphore_wait(barrier, 1 + has_up.astype(jnp.int32) + has_down.astype(jnp.int32))

    def up(d, source):
        return pltpu.make_async_remote_copy(
            src_ref=source,
            dst_ref=held.at[d + 2],
            send_sem=up_sem.at[d],
            recv_sem=recv_sem.at[d + 2],
            device_id={"sp": me + 2},
            device_id_type=MESH,
        )

    def side(d, slot, source):
        return pltpu.make_async_remote_copy(
            src_ref=source,
            dst_ref=held.at[slot],
            send_sem=side_sem.at[d],
            recv_sem=recv_sem.at[slot],
            device_id={"sp": partner},
            device_id_type=MESH,
        )

    def send(d, source):
        pl.when(has_up)(lambda: up(d, source).start())
        pl.when(odd == 0)(lambda: side(d, d + 1, source).start())
        pl.when((odd == 1) & (d >= 2))(lambda: side(d, d - 1, source).start())

    width = heads * HEAD_DIM
    row_width = 2 * width
    lane = lax.broadcasted_iota(jnp.int32, (QUERY_ROWS, width), 1)
    tile_blocks = SPAN // BLOCK

    def bias_row(bias_rows, h, start):
        step = min(row_width, BLOCK)
        pieces = []
        for first in range(0, BLOCK, step):
            flat = h * length + start + first
            row, col = flat // row_width, flat % row_width
            pieces.append(bias_rows[row : row + 1, col : col + step])
        return jnp.concatenate(pieces, axis=1) if len(pieces) > 1 else pieces[0]

    def tile(source, span, q0, masked):
        k0 = span * SPAN
        key_rows = source[k0 : k0 + SPAN, :width]
        value_rows = source[k0 : k0 + SPAN, width:row_width]
        bias_rows = source[length : length + BIAS_ROWS, :].astype(jnp.float32)
        gathered = None
        for h in range(heads):
            query = q_ref[h, pl.ds(q0, QUERY_ROWS), :]
            later = jnp.zeros((QUERY_ROWS, 1), jnp.float32)
            weights = [None] * tile_blocks
            for block in reversed(range(tile_blocks)):
                b0 = block * BLOCK
                scores = lax.dot_general(
                    query,
                    key_rows[b0 : b0 + BLOCK],
                    (((1,), (1,)), ((), ())),
                    preferred_element_type=jnp.float32,
                )
                scores = scores + bias_row(bias_rows, h, k0 + b0)
                soft = jnp.maximum(scores, 0.0) + jnp.log(1.0 + jnp.exp(-jnp.abs(scores)))
                rest = scores - soft
                if masked:
                    q_pos = q0 - k0 + lax.broadcasted_iota(jnp.int32, scores.shape, 0)
                    k_pos = b0 + lax.broadcasted_iota(jnp.int32, scores.shape, 1)
                    earlier = k_pos < q_pos
                    soft = jnp.where(earlier, soft, 0.0)
                high = soft.astype(jnp.bfloat16)
                low = (soft - high.astype(jnp.float32)).astype(jnp.bfloat16)
                beyond = jnp.dot(high, tri[...], preferred_element_type=jnp.float32) + jnp.dot(
                    low, tri[...], preferred_element_type=jnp.float32
                )
                beyond = beyond + later
                piece = jnp.exp(rest - beyond)
                if masked:
                    piece = jnp.where(earlier, piece, 0.0)
                weights[block] = piece.astype(jnp.bfloat16)
                later = beyond[:, :1] + soft[:, :1]
            joined = jnp.concatenate(weights, axis=1)
            span_out = jnp.dot(joined, value_rows, preferred_element_type=jnp.float32)
            rows = pl.ds(q0, QUERY_ROWS)
            held_after = after[h, rows, :]
            span_out = jnp.exp(-held_after[:, :width]) * span_out
            after[h, rows, :] = held_after + later
            if gathered is None:
                gathered = span_out
            else:
                gathered = jnp.where(lane >= h * HEAD_DIM, span_out, gathered)
        rows = pl.ds(q0, QUERY_ROWS)
        total[rows, :] = total[rows, :] + gathered

    span_count = length // SPAN

    def compute(source, own):
        def chunk(c, carry):
            q0 = pl.multiple_of(c * QUERY_ROWS, QUERY_ROWS)
            for span in reversed(range(span_count)):
                if own:
                    span_of = q0 // SPAN
                    pl.when(span_of == span)(lambda: tile(source, span, q0, True))
                    if span < span_count - 1:
                        pl.when(span_of > span)(lambda: tile(source, span, q0, False))
                else:
                    tile(source, span, q0, False)
            return carry

        lax.fori_loop(0, length // QUERY_ROWS, chunk, 0)

    send(0, own_ref)
    compute(own_ref, True)

    def arrive(d, carry):
        pltpu.make_async_remote_copy(
            src_ref=held.at[d],
            dst_ref=held.at[d],
            send_sem=up_sem.at[d],
            recv_sem=recv_sem.at[d],
            device_id={"sp": partner},
            device_id_type=MESH,
        ).wait_recv()
        pl.when(lax.rem(d, 2) == 0)(lambda: send(d, held.at[d]))
        compute(held.at[d], False)
        return carry

    lax.fori_loop(1, me + 1, arrive, 0)
    out_ref[...] = total[...].astype(jnp.bfloat16)

    def sent(d, source):
        pl.when(has_up)(lambda: up(d, source).wait_send())
        pl.when(odd == 0)(lambda: side(d, d + 1, source).wait_send())
        pl.when((odd == 1) & (d >= 2))(lambda: side(d, d - 1, source).wait_send())

    sent(0, own_ref)

    def drain(half, carry):
        sent(2 * half, held.at[2 * half])
        return carry

    lax.fori_loop(1, me // 2 + 1, drain, 0)


def attend(queries, keys, values, key_bias):
    n = lax.axis_size("sp")
    length = queries.shape[0]
    heads = key_bias.shape[1]
    width = heads * HEAD_DIM
    row_width = 2 * width
    head_of = lax.iota(jnp.int32, width) // HEAD_DIM
    scaled = queries * jnp.bfloat16(HEAD_DIM ** (-0.5))
    per_head = jnp.where(
        head_of[None, None, :] == lax.iota(jnp.int32, heads)[:, None, None],
        scaled[None],
        jnp.bfloat16(0),
    )
    bias_rows = jnp.transpose(key_bias).reshape(-1, row_width)
    bias_rows = jnp.pad(bias_rows, ((0, BIAS_ROWS - bias_rows.shape[0]), (0, 0)))
    own = jnp.concatenate([jnp.concatenate([keys, values], axis=1), bias_rows], axis=0)
    vmem = pl.BlockSpec(memory_space=pltpu.VMEM)
    return pl.pallas_call(
        functools.partial(attend_kernel, n, length, heads),
        out_shape=jax.ShapeDtypeStruct((length, width), jnp.bfloat16),
        in_specs=[vmem, vmem],
        out_specs=vmem,
        scratch_shapes=[
            pltpu.VMEM((n, length + BIAS_ROWS, row_width), jnp.bfloat16),
            pltpu.VMEM((length, width), jnp.float32),
            pltpu.VMEM((heads, length, 128), jnp.float32),
            pltpu.VMEM((BLOCK, BLOCK), jnp.bfloat16),
            pltpu.SemaphoreType.DMA((n + 2,)),
            pltpu.SemaphoreType.DMA((n + 2,)),
            pltpu.SemaphoreType.DMA((n + 2,)),
        ],
        compiler_params=pltpu.CompilerParams(
            collective_id=0, has_side_effects=True, vmem_limit_bytes=40 * 1024 * 1024
        ),
        name="attend",
    )(per_head, own)


def dispatch_kernel(
    n, groups, outgoing, gate_hbm, up_hbm, down_hbm, partial, rows, block, hidden, gate, up, down,
    weight_sem, sp_sem, chip_sem, core_sem, recv_sem,
):
    me, my_t = lax.axis_index("sp"), lax.axis_index("tp")
    mate = my_t + 1 - 2 * lax.rem(my_t, 2)
    chips = groups // 2
    alike = [lax.rem(my_t + 2 * k, groups) for k in range(1, chips)]
    loads = [
        pltpu.make_async_copy(gate_hbm, gate, weight_sem.at[0]),
        pltpu.make_async_copy(up_hbm, up, weight_sem.at[1]),
        pltpu.make_async_copy(down_hbm, down, weight_sem.at[2]),
    ]
    for load in loads:
        load.start()
    greet_all(n, me, mate, alike)
    capacity = outgoing.shape[1]

    def copy(source, t, s, send_sem, device):
        return pltpu.make_async_remote_copy(
            src_ref=source,
            dst_ref=rows.at[t * n + s],
            send_sem=send_sem,
            recv_sem=recv_sem.at[t * n + s],
            device_id=device,
            device_id_type=MESH,
        )

    def to_expert(r):
        target = lax.rem(me + r, n)
        return copy(outgoing.at[target], my_t, me, sp_sem.at[r], {"sp": target})

    def to_chip(k, s, source):
        return copy(source, my_t, s, chip_sem.at[k * n + s], {"tp": alike[k]})

    def to_mate(t, s, source):
        return copy(source, t, s, core_sem.at[t * n + s], {"tp": mate})

    def arrived(t, s):
        copy(rows.at[t * n + s], t, s, core_sem.at[t * n + s], {"tp": mate}).wait_recv()

    def spread(s, source):
        for k in range(chips - 1):
            to_chip(k, s, source).start()
        to_mate(my_t, s, source).start()

    def relay(r):
        s = lax.rem(me + n - r, n)
        for t in alike:
            arrived(t, s)
            to_mate(t, s, rows.at[t * n + s]).start()

    def issue(r, carry):
        to_expert(r).start()
        return carry

    spread(me, outgoing.at[me])
    lax.fori_loop(1, n, issue, 0)
    rows[my_t * n + me] = outgoing[me]

    def expert(r):
        s = lax.rem(me + n - r, n)
        arrived(mate, s)
        for t in alike:
            arrived(t + 1 - 2 * lax.rem(t, 2), s)
        block[...] = jnp.concatenate([rows[t * n + s] for t in range(groups)], axis=0)

        def units(f, carry):
            columns = pl.ds(pl.multiple_of(f * BLOCK, BLOCK), BLOCK)
            gate_act = jnp.dot(block[...], gate[:, columns], preferred_element_type=jnp.float32)
            up_act = jnp.dot(block[...], up[:, columns], preferred_element_type=jnp.float32)
            silu = gate_act / (1.0 + jnp.exp(-gate_act))
            hidden[:, columns] = (silu * up_act).astype(jnp.bfloat16)
            return carry

        lax.fori_loop(0, gate.shape[1] // BLOCK, units, 0)

        def features(f, carry):
            columns = pl.ds(pl.multiple_of(f * BLOCK, BLOCK), BLOCK)
            value = jnp.dot(hidden[...], down[:, columns], preferred_element_type=jnp.float32)
            for t in range(groups):
                piece = value[t * capacity : (t + 1) * capacity]
                partial[t * n + s, :, columns] = piece.astype(jnp.bfloat16)
            return carry

        lax.fori_loop(0, down.shape[1] // BLOCK, features, 0)

    def step(r, carry):
        s = lax.rem(me + n - r, n)
        arrived(my_t, s)
        spread(s, rows.at[my_t * n + s])
        relay(r - 1)
        pl.when(r >= 2)(lambda: expert(r - 2))
        return carry

    lax.fori_loop(1, 2, step, 0)
    for load in loads:
        load.wait()
    lax.fori_loop(2, n, step, 0)
    relay(n - 1)

    def last(r, carry):
        expert(r)
        return carry

    lax.fori_loop(n - 2, n, last, 0)

    def finish(s, carry):
        pl.when(s >= 1)(lambda: to_expert(s).wait_send())
        for k in range(chips - 1):
            to_chip(k, s, outgoing.at[me]).wait_send()
            to_mate(alike[k], s, outgoing.at[me]).wait_send()
        to_mate(my_t, s, outgoing.at[me]).wait_send()
        return carry

    lax.fori_loop(0, n, finish, 0)


def greet_all(n, me, mate, alike):
    barrier = pltpu.get_barrier_semaphore()

    def greet(device):
        pl.semaphore_signal(barrier, inc=1, device_id=device, device_id_type=MESH)

    def greet_sp(r, carry):
        greet({"sp": lax.rem(me + r, n)})
        return carry

    lax.fori_loop(1, n, greet_sp, 0)
    greet({"tp": mate})
    for t in alike:
        greet({"tp": t})
    pl.semaphore_wait(barrier, n + len(alike))


def combine_kernel(
    n, groups, partial, back, pair, other, done, pair_send, pair_recv, chip_send, chip_recv,
    back_send, back_recv,
):
    me, my_t = lax.axis_index("sp"), lax.axis_index("tp")
    core = lax.rem(my_t, 2)
    mate = my_t + 1 - 2 * core
    chips = groups // 2
    alike = [lax.rem(my_t + 2 * k, groups) for k in range(1, chips)]
    greet_all(n, me, mate, alike)

    def home(r):
        return lax.rem(me + 1 + r, n)

    def pair_copy(chip, r):
        return pltpu.make_async_remote_copy(
            src_ref=partial.at[(2 * chip + 1 - core) * n + home(r)],
            dst_ref=pair.at[chip * n + r],
            send_sem=pair_send.at[chip * n + r],
            recv_sem=pair_recv.at[chip * n + r],
            device_id={"tp": mate},
            device_id_type=MESH,
        )

    def chip_copy(k, r):
        return pltpu.make_async_remote_copy(
            src_ref=pair.at[(alike[k] // 2) * n + r],
            dst_ref=other.at[k * n + r],
            send_sem=chip_send.at[k * n + r],
            recv_sem=chip_recv.at[k * n + r],
            device_id={"tp": alike[k]},
            device_id_type=MESH,
        )

    def back_copy(r):
        return pltpu.make_async_remote_copy(
            src_ref=done.at[r],
            dst_ref=back.at[me],
            send_sem=back_send.at[r],
            recv_sem=back_recv.at[me],
            device_id={"sp": home(r)},
            device_id_type=MESH,
        )

    def start_pairs(r, carry):
        for chip in range(chips):
            pair_copy(chip, r).start()
        return carry

    lax.fori_loop(0, n, start_pairs, 0)

    def add_pairs(r):
        for chip in range(chips):
            pair_copy(chip, r).wait_recv()
        for k in range(chips - 1):
            chip = alike[k] // 2
            pair[chip * n + r] = (
                partial[alike[k] * n + home(r)].astype(jnp.float32)
                + pair[chip * n + r].astype(jnp.float32)
            ).astype(jnp.bfloat16)

    def add_chips(r):
        value = partial[my_t * n + home(r)].astype(jnp.float32) + pair[
            (my_t // 2) * n + r
        ].astype(jnp.float32)
        for k in range(chips - 1):
            chip_copy(k, r).wait_recv()
            value = value + other[k * n + r].astype(jnp.float32)
        return value.astype(jnp.bfloat16)

    def send_chips(r):
        for k in range(chips - 1):
            chip_copy(k, r).start()

    lag = 1
    for r in range(lag):
        add_pairs(r)
        send_chips(r)

    def step(r, carry):
        add_pairs(r)
        send_chips(r)
        done[r - lag] = add_chips(r - lag)
        back_copy(r - lag).start()
        return carry

    lax.fori_loop(lag, n, step, 0)
    for r in range(n - lag, n):
        if r == n - 1:
            back[me] = add_chips(r)
        else:
            done[r] = add_chips(r)
            back_copy(r).start()

    def finish(r, carry):
        for chip in range(chips):
            pair_copy(chip, r).wait_send()
        for k in range(chips - 1):
            chip_copy(k, r).wait_send()
        return carry

    lax.fori_loop(0, n, finish, 0)

    def finish_back(r, carry):
        back_copy(r).wait_send()
        source = home(r)
        pltpu.make_async_remote_copy(
            src_ref=done.at[r],
            dst_ref=back.at[source],
            send_sem=back_send.at[r],
            recv_sem=back_recv.at[source],
            device_id={"sp": source},
            device_id_type=MESH,
        ).wait_recv()
        return carry

    lax.fori_loop(0, n - 1, finish_back, 0)


def dispatch(outgoing, gate, up, down):
    n, groups = lax.axis_size("sp"), lax.axis_size("tp")
    chips = groups // 2
    _, capacity, width = outgoing.shape
    units = gate.shape[1]
    vmem = pl.BlockSpec(memory_space=pltpu.VMEM)
    anywhere = pl.BlockSpec(memory_space=pl.ANY)
    return pl.pallas_call(
        functools.partial(dispatch_kernel, n, groups),
        out_shape=jax.ShapeDtypeStruct((groups * n, capacity, width), outgoing.dtype),
        in_specs=[vmem, anywhere, anywhere, anywhere],
        out_specs=vmem,
        scratch_shapes=[
            pltpu.VMEM((groups * n, capacity, width), outgoing.dtype),
            pltpu.VMEM((groups * capacity, width), outgoing.dtype),
            pltpu.VMEM((groups * capacity, units), outgoing.dtype),
            pltpu.VMEM((width, units), gate.dtype),
            pltpu.VMEM((width, units), up.dtype),
            pltpu.VMEM((units, width), down.dtype),
            pltpu.SemaphoreType.DMA((3,)),
            pltpu.SemaphoreType.DMA((n,)),
            pltpu.SemaphoreType.DMA((max(1, chips - 1) * n,)),
            pltpu.SemaphoreType.DMA((groups * n,)),
            pltpu.SemaphoreType.DMA((groups * n,)),
        ],
        compiler_params=pltpu.CompilerParams(
            collective_id=1, has_side_effects=True, vmem_limit_bytes=60 * 1024 * 1024
        ),
        name="dispatch",
    )(outgoing, gate, up, down)


def combine(partial):
    n, groups = lax.axis_size("sp"), lax.axis_size("tp")
    chips = groups // 2
    _, capacity, width = partial.shape
    vmem = pl.BlockSpec(memory_space=pltpu.VMEM)
    apart = max(1, chips - 1) * n
    return pl.pallas_call(
        functools.partial(combine_kernel, n, groups),
        out_shape=jax.ShapeDtypeStruct((n, capacity, width), partial.dtype),
        in_specs=[vmem],
        out_specs=vmem,
        scratch_shapes=[
            pltpu.VMEM((chips * n, capacity, width), partial.dtype),
            pltpu.VMEM((apart, capacity, width), partial.dtype),
            pltpu.VMEM((n, capacity, width), partial.dtype),
            pltpu.SemaphoreType.DMA((chips * n,)),
            pltpu.SemaphoreType.DMA((chips * n,)),
            pltpu.SemaphoreType.DMA((apart,)),
            pltpu.SemaphoreType.DMA((apart,)),
            pltpu.SemaphoreType.DMA((n,)),
            pltpu.SemaphoreType.DMA((n,)),
        ],
        compiler_params=pltpu.CompilerParams(
            collective_id=2, has_side_effects=True, vmem_limit_bytes=56 * 1024 * 1024
        ),
        name="combine",
    )(partial)


def shards(
    queries,
    keys,
    values,
    key_bias,
    residual,
    out_weight,
    norm_gain,
    routes,
    route_weights,
    gate_weight,
    up_weight,
    down_weight,
):
    sp_count = lax.axis_size("sp")
    attended = attend(queries, keys, values, key_bias)
    token_heads = lax.all_to_all(attended, "tp", split_axis=0, concat_axis=1, tiled=True)
    projected = jnp.dot(token_heads, out_weight, preferred_element_type=jnp.float32)
    stream = (residual.astype(jnp.float32) + projected).astype(jnp.bfloat16).astype(jnp.float32)
    normed = (
        stream * lax.rsqrt(jnp.mean(stream * stream, axis=-1, keepdims=True) + epsilon) * norm_gain
    ).astype(jnp.bfloat16)
    token_count = residual.shape[0]
    width_model = residual.shape[1]
    capacity = max(2, 5 * token_count * TOP // (4 * sp_count))
    flat_routes = routes.reshape(-1)
    onehot = (flat_routes[:, None] == lax.iota(jnp.int32, sp_count)[None, :]).astype(jnp.int32)
    before = jnp.cumsum(onehot, axis=0) - onehot
    slot_of = flat_routes * capacity + jnp.sum(before * onehot, axis=1)
    select = (slot_of[:, None] == lax.iota(jnp.int32, sp_count * capacity)[None, :]).astype(
        jnp.bfloat16
    )
    placing = jnp.sum(select.reshape(token_count, TOP, sp_count * capacity), axis=1)
    outgoing = jnp.einsum("ts,td->sd", placing, normed, preferred_element_type=jnp.float32).astype(
        jnp.bfloat16
    )
    partial_rows = dispatch(
        outgoing.reshape(sp_count, capacity, width_model),
        gate_weight[0],
        up_weight[0],
        down_weight[0],
    )
    returned = combine(partial_rows).reshape(-1, width_model)
    picked = jnp.dot(select, returned, preferred_element_type=jnp.float32).reshape(
        token_count, TOP, width_model
    )
    routed = jnp.sum(picked * route_weights[:, :, None], axis=1)
    return (stream + routed).astype(jnp.bfloat16)


def solution(mesh):
    return jax.shard_map(
        shards,
        mesh=mesh,
        in_specs=(
            P("sp", "tp"),
            P("sp", "tp"),
            P("sp", "tp"),
            P("sp", "tp"),
            P(("sp", "tp"), None),
            P(),
            P(),
            P(("sp", "tp"), None),
            P(("sp", "tp"), None),
            P("sp", None, "tp"),
            P("sp", None, "tp"),
            P("sp", "tp", None),
        ),
        out_specs=P(("sp", "tp"), None),
        check_vma=False,
    )
```

```python
import functools

import jax
import jax.numpy as jnp
from jax import lax
from jax.experimental import pallas as pl
from jax.experimental.pallas import tpu as pltpu
from jax.sharding import PartitionSpec as P

HEAD_DIM = 64
TOP = 2
SPAN = 512
BLOCK = 256
QUERY_ROWS = 256
BIAS_ROWS = 16
MESH = pl.DeviceIdType.MESH


epsilon = 1e-06


def attend_kernel(
    n, length, heads, q_ref, own_ref, out_ref, held, total, after, tri, up_sem, side_sem, recv_sem
):
    me = lax.axis_index("sp")
    odd = lax.rem(me, 2)
    partner = me + 1 - 2 * odd
    has_up = me + 2 < n
    has_down = me >= 2
    barrier = pltpu.get_barrier_semaphore()

    def greet(device):
        pl.semaphore_signal(barrier, inc=1, device_id={"sp": device}, device_id_type=MESH)

    greet(partner)
    pl.when(has_up)(lambda: greet(me + 2))
    pl.when(has_down)(lambda: greet(me - 2))

    total[...] = jnp.zeros_like(total)
    after[...] = jnp.zeros_like(after)
    tri_row = lax.broadcasted_iota(jnp.int32, (BLOCK, BLOCK), 0)
    tri_col = lax.broadcasted_iota(jnp.int32, (BLOCK, BLOCK), 1)
    tri[...] = (tri_row > tri_col).astype(jnp.float32).astype(jnp.bfloat16)

    pl.semaphore_wait(barrier, 1 + has_up.astype(jnp.int32) + has_down.astype(jnp.int32))

    def up(d, source):
        return pltpu.make_async_remote_copy(
            src_ref=source,
            dst_ref=held.at[d + 2],
            send_sem=up_sem.at[d],
            recv_sem=recv_sem.at[d + 2],
            device_id={"sp": me + 2},
            device_id_type=MESH,
        )

    def side(d, slot, source):
        return pltpu.make_async_remote_copy(
            src_ref=source,
            dst_ref=held.at[slot],
            send_sem=side_sem.at[d],
            recv_sem=recv_sem.at[slot],
            device_id={"sp": partner},
            device_id_type=MESH,
        )

    def send(d, source):
        pl.when(has_up)(lambda: up(d, source).start())
        pl.when(odd == 0)(lambda: side(d, d + 1, source).start())
        pl.when((odd == 1) & (d >= 2))(lambda: side(d, d - 1, source).start())

    width = heads * HEAD_DIM
    row_width = 2 * width
    lane = lax.broadcasted_iota(jnp.int32, (QUERY_ROWS, width), 1)
    tile_blocks = SPAN // BLOCK

    def bias_row(bias_rows, h, start):
        step = min(row_width, BLOCK)
        pieces = []
        for first in range(0, BLOCK, step):
            flat = h * length + start + first
            row, col = flat // row_width, flat % row_width
            pieces.append(bias_rows[row : row + 1, col : col + step])
        return jnp.concatenate(pieces, axis=1) if len(pieces) > 1 else pieces[0]

    def tile(source, span, q0, masked):
        k0 = span * SPAN
        key_rows = source[k0 : k0 + SPAN, :width]
        value_rows = source[k0 : k0 + SPAN, width:row_width]
        bias_rows = source[length : length + BIAS_ROWS, :].astype(jnp.float32)
        gathered = None
        for h in range(heads):
            query = q_ref[h, pl.ds(q0, QUERY_ROWS), :]
            later = jnp.zeros((QUERY_ROWS, 1), jnp.float32)
            weights = [None] * tile_blocks
            for block in reversed(range(tile_blocks)):
                b0 = block * BLOCK
                scores = lax.dot_general(
                    query,
                    key_rows[b0 : b0 + BLOCK],
                    (((1,), (1,)), ((), ())),
                    preferred_element_type=jnp.float32,
                )
                scores = scores + bias_row(bias_rows, h, k0 + b0)
                soft = jnp.maximum(scores, 0.0) + jnp.log(1.0 + jnp.exp(-jnp.abs(scores)))
                rest = scores - soft
                if masked:
                    q_pos = q0 - k0 + lax.broadcasted_iota(jnp.int32, scores.shape, 0)
                    k_pos = b0 + lax.broadcasted_iota(jnp.int32, scores.shape, 1)
                    earlier = k_pos < q_pos
                    soft = jnp.where(earlier, soft, 0.0)
                high = soft.astype(jnp.bfloat16)
                low = (soft - high.astype(jnp.float32)).astype(jnp.bfloat16)
                beyond = jnp.dot(high, tri[...], preferred_element_type=jnp.float32) + jnp.dot(
                    low, tri[...], preferred_element_type=jnp.float32
                )
                beyond = beyond + later
                piece = jnp.exp(rest - beyond)
                if masked:
                    piece = jnp.where(earlier, piece, 0.0)
                weights[block] = piece.astype(jnp.bfloat16)
                later = beyond[:, :1] + soft[:, :1]
            joined = jnp.concatenate(weights, axis=1)
            span_out = jnp.dot(joined, value_rows, preferred_element_type=jnp.float32)
            rows = pl.ds(q0, QUERY_ROWS)
            held_after = after[h, rows, :]
            span_out = jnp.exp(-held_after[:, :width]) * span_out
            after[h, rows, :] = held_after + later
            if gathered is None:
                gathered = span_out
            else:
                gathered = jnp.where(lane >= h * HEAD_DIM, span_out, gathered)
        rows = pl.ds(q0, QUERY_ROWS)
        total[rows, :] = total[rows, :] + gathered

    span_count = length // SPAN

    def compute(source, own):
        def chunk(c, carry):
            q0 = pl.multiple_of(c * QUERY_ROWS, QUERY_ROWS)
            for span in reversed(range(span_count)):
                if own:
                    span_of = q0 // SPAN
                    pl.when(span_of == span)(lambda: tile(source, span, q0, True))
                    if span < span_count - 1:
                        pl.when(span_of > span)(lambda: tile(source, span, q0, False))
                else:
                    tile(source, span, q0, False)
            return carry

        lax.fori_loop(0, length // QUERY_ROWS, chunk, 0)

    send(0, own_ref)
    compute(own_ref, True)

    def arrive(d, carry):
        pltpu.make_async_remote_copy(
            src_ref=held.at[d],
            dst_ref=held.at[d],
            send_sem=up_sem.at[d],
            recv_sem=recv_sem.at[d],
            device_id={"sp": partner},
            device_id_type=MESH,
        ).wait_recv()
        pl.when(lax.rem(d, 2) == 0)(lambda: send(d, held.at[d]))
        compute(held.at[d], False)
        return carry

    lax.fori_loop(1, me + 1, arrive, 0)
    out_ref[...] = total[...].astype(jnp.bfloat16)

    def sent(d, source):
        pl.when(has_up)(lambda: up(d, source).wait_send())
        pl.when(odd == 0)(lambda: side(d, d + 1, source).wait_send())
        pl.when((odd == 1) & (d >= 2))(lambda: side(d, d - 1, source).wait_send())

    sent(0, own_ref)

    def drain(half, carry):
        sent(2 * half, held.at[2 * half])
        return carry

    lax.fori_loop(1, me // 2 + 1, drain, 0)


def attend(queries, keys, values, key_bias):
    n = lax.axis_size("sp")
    length = queries.shape[0]
    heads = key_bias.shape[1]
    width = heads * HEAD_DIM
    row_width = 2 * width
    head_of = lax.iota(jnp.int32, width) // HEAD_DIM
    scaled = queries * jnp.bfloat16(HEAD_DIM ** (-0.5))
    per_head = jnp.where(
        head_of[None, None, :] == lax.iota(jnp.int32, heads)[:, None, None],
        scaled[None],
        jnp.bfloat16(0),
    )
    bias_rows = jnp.transpose(key_bias).reshape(-1, row_width)
    bias_rows = jnp.pad(bias_rows, ((0, BIAS_ROWS - bias_rows.shape[0]), (0, 0)))
    own = jnp.concatenate([jnp.concatenate([keys, values], axis=1), bias_rows], axis=0)
    vmem = pl.BlockSpec(memory_space=pltpu.VMEM)
    return pl.pallas_call(
        functools.partial(attend_kernel, n, length, heads),
        out_shape=jax.ShapeDtypeStruct((length, width), jnp.bfloat16),
        in_specs=[vmem, vmem],
        out_specs=vmem,
        scratch_shapes=[
            pltpu.VMEM((n, length + BIAS_ROWS, row_width), jnp.bfloat16),
            pltpu.VMEM((length, width), jnp.float32),
            pltpu.VMEM((heads, length, 128), jnp.float32),
            pltpu.VMEM((BLOCK, BLOCK), jnp.bfloat16),
            pltpu.SemaphoreType.DMA((n + 2,)),
            pltpu.SemaphoreType.DMA((n + 2,)),
            pltpu.SemaphoreType.DMA((n + 2,)),
        ],
        compiler_params=pltpu.CompilerParams(
            collective_id=0, has_side_effects=True, vmem_limit_bytes=40 * 1024 * 1024
        ),
        name="attend",
    )(per_head, own)


def dispatch_kernel(
    n, groups, outgoing, gate_hbm, up_hbm, down_hbm, back, partial, rows, block, hidden, gate, up,
    down, pair, other, done, weight_sem, sp_sem, chip_sem, core_sem, recv_sem, pair_send, pair_recv,
    chip_send, chip_recv, back_send, back_recv,
):
    me, my_t = lax.axis_index("sp"), lax.axis_index("tp")
    core = lax.rem(my_t, 2)
    mate = my_t + 1 - 2 * core
    chips = groups // 2
    alike = [lax.rem(my_t + 2 * k, groups) for k in range(1, chips)]
    loads = [
        pltpu.make_async_copy(gate_hbm, gate, weight_sem.at[0]),
        pltpu.make_async_copy(up_hbm, up, weight_sem.at[1]),
        pltpu.make_async_copy(down_hbm, down, weight_sem.at[2]),
    ]
    for load in loads:
        load.start()
    greet_all(n, me, mate, alike)
    capacity = outgoing.shape[1]

    def copy(source, t, s, send_sem, device):
        return pltpu.make_async_remote_copy(
            src_ref=source,
            dst_ref=rows.at[t * n + s],
            send_sem=send_sem,
            recv_sem=recv_sem.at[t * n + s],
            device_id=device,
            device_id_type=MESH,
        )

    def to_expert(r):
        target = lax.rem(me + r, n)
        return copy(outgoing.at[target], my_t, me, sp_sem.at[r], {"sp": target})

    def to_chip(k, s, source):
        return copy(source, my_t, s, chip_sem.at[k * n + s], {"tp": alike[k]})

    def to_mate(t, s, source):
        return copy(source, t, s, core_sem.at[t * n + s], {"tp": mate})

    def arrived(t, s):
        copy(rows.at[t * n + s], t, s, core_sem.at[t * n + s], {"tp": mate}).wait_recv()

    def spread(s, source):
        for k in range(chips - 1):
            to_chip(k, s, source).start()
        to_mate(my_t, s, source).start()

    def relay(r):
        s = lax.rem(me + n - r, n)
        for t in alike:
            arrived(t, s)
            to_mate(t, s, rows.at[t * n + s]).start()

    def issue(r, carry):
        to_expert(r).start()
        return carry

    spread(me, outgoing.at[me])
    lax.fori_loop(1, n, issue, 0)
    rows[my_t * n + me] = outgoing[me]

    def expert(r):
        s = lax.rem(me + n - r, n)
        arrived(mate, s)
        for t in alike:
            arrived(t + 1 - 2 * lax.rem(t, 2), s)
        block[...] = jnp.concatenate([rows[t * n + s] for t in range(groups)], axis=0)

        def units(f, carry):
            columns = pl.ds(pl.multiple_of(f * BLOCK, BLOCK), BLOCK)
            gate_act = jnp.dot(block[...], gate[:, columns], preferred_element_type=jnp.float32)
            up_act = jnp.dot(block[...], up[:, columns], preferred_element_type=jnp.float32)
            silu = gate_act / (1.0 + jnp.exp(-gate_act))
            hidden[:, columns] = (silu * up_act).astype(jnp.bfloat16)
            return carry

        lax.fori_loop(0, gate.shape[1] // BLOCK, units, 0)

        def features(f, carry):
            columns = pl.ds(pl.multiple_of(f * BLOCK, BLOCK), BLOCK)
            value = jnp.dot(hidden[...], down[:, columns], preferred_element_type=jnp.float32)
            for t in range(groups):
                piece = value[t * capacity : (t + 1) * capacity]
                partial[t * n + s, :, columns] = piece.astype(jnp.bfloat16)
            return carry

        lax.fori_loop(0, down.shape[1] // BLOCK, features, 0)

    def home(r):
        return lax.rem(me + n - r, n)

    def pair_copy(chip, r):
        return pltpu.make_async_remote_copy(
            src_ref=partial.at[(2 * chip + 1 - core) * n + home(r)],
            dst_ref=pair.at[chip * n + r],
            send_sem=pair_send.at[chip * n + r],
            recv_sem=pair_recv.at[chip * n + r],
            device_id={"tp": mate},
            device_id_type=MESH,
        )

    def chip_copy(k, r):
        return pltpu.make_async_remote_copy(
            src_ref=pair.at[(alike[k] // 2) * n + r],
            dst_ref=other.at[k * n + r],
            send_sem=chip_send.at[k * n + r],
            recv_sem=chip_recv.at[k * n + r],
            device_id={"tp": alike[k]},
            device_id_type=MESH,
        )

    def back_copy(r):
        return pltpu.make_async_remote_copy(
            src_ref=done.at[r],
            dst_ref=back.at[me],
            send_sem=back_send.at[r],
            recv_sem=back_recv.at[me],
            device_id={"sp": home(r)},
            device_id_type=MESH,
        )

    def add_pairs(r):
        for chip in range(chips):
            pair_copy(chip, r).wait_recv()
        for k in range(chips - 1):
            chip = alike[k] // 2
            pair[chip * n + r] = (
                partial[alike[k] * n + home(r)].astype(jnp.float32)
                + pair[chip * n + r].astype(jnp.float32)
            ).astype(jnp.bfloat16)

    def add_chips(r):
        value = partial[my_t * n + home(r)].astype(jnp.float32) + pair[
            (my_t // 2) * n + r
        ].astype(jnp.float32)
        for k in range(chips - 1):
            chip_copy(k, r).wait_recv()
            value = value + other[k * n + r].astype(jnp.float32)
        return value.astype(jnp.bfloat16)

    def send_chips(r):
        for k in range(chips - 1):
            chip_copy(k, r).start()

    def multiply(r):
        expert(r)
        for chip in range(chips):
            pair_copy(chip, r).start()

    def sum_pairs(r):
        add_pairs(r)
        send_chips(r)

    def give_own():
        back[me] = add_chips(0)

    def give_back(r):
        done[r] = add_chips(r)
        back_copy(r).start()

    def flow(r):
        pl.when(r < n)(lambda: multiply(r))
        pl.when((r >= 1) & (r <= n))(lambda: sum_pairs(r - 1))
        pl.when(r == 2)(give_own)
        pl.when(r >= 3)(lambda: give_back(r - 2))

    def step(r, carry):
        s = lax.rem(me + n - r, n)
        arrived(my_t, s)
        spread(s, rows.at[my_t * n + s])
        relay(r - 1)
        pl.when(r >= 2)(lambda: flow(r - 2))
        return carry

    lax.fori_loop(1, 2, step, 0)
    for load in loads:
        load.wait()
    lax.fori_loop(2, n, step, 0)
    relay(n - 1)

    def last(r, carry):
        flow(r)
        return carry

    lax.fori_loop(n - 2, n + 2, last, 0)

    def finish(s, carry):
        pl.when(s >= 1)(lambda: to_expert(s).wait_send())
        for k in range(chips - 1):
            to_chip(k, s, outgoing.at[me]).wait_send()
            to_mate(alike[k], s, outgoing.at[me]).wait_send()
        to_mate(my_t, s, outgoing.at[me]).wait_send()
        return carry

    lax.fori_loop(0, n, finish, 0)

    def finish_sums(r, carry):
        for chip in range(chips):
            pair_copy(chip, r).wait_send()
        for k in range(chips - 1):
            chip_copy(k, r).wait_send()
        return carry

    lax.fori_loop(0, n, finish_sums, 0)

    def finish_back(r, carry):
        back_copy(r).wait_send()
        source = home(r)
        pltpu.make_async_remote_copy(
            src_ref=done.at[r],
            dst_ref=back.at[source],
            send_sem=back_send.at[r],
            recv_sem=back_recv.at[source],
            device_id={"sp": source},
            device_id_type=MESH,
        ).wait_recv()
        return carry

    lax.fori_loop(1, n, finish_back, 0)


def greet_all(n, me, mate, alike):
    barrier = pltpu.get_barrier_semaphore()

    def greet(device):
        pl.semaphore_signal(barrier, inc=1, device_id=device, device_id_type=MESH)

    def greet_sp(r, carry):
        greet({"sp": lax.rem(me + r, n)})
        return carry

    lax.fori_loop(1, n, greet_sp, 0)
    greet({"tp": mate})
    for t in alike:
        greet({"tp": t})
    pl.semaphore_wait(barrier, n + len(alike))


def dispatch(outgoing, gate, up, down):
    n, groups = lax.axis_size("sp"), lax.axis_size("tp")
    chips = groups // 2
    _, capacity, width = outgoing.shape
    units = gate.shape[1]
    apart = max(1, chips - 1) * n
    vmem = pl.BlockSpec(memory_space=pltpu.VMEM)
    anywhere = pl.BlockSpec(memory_space=pl.ANY)
    return pl.pallas_call(
        functools.partial(dispatch_kernel, n, groups),
        out_shape=jax.ShapeDtypeStruct((n, capacity, width), outgoing.dtype),
        in_specs=[vmem, anywhere, anywhere, anywhere],
        out_specs=vmem,
        scratch_shapes=[
            pltpu.VMEM((groups * n, capacity, width), outgoing.dtype),
            pltpu.VMEM((groups * n, capacity, width), outgoing.dtype),
            pltpu.VMEM((groups * capacity, width), outgoing.dtype),
            pltpu.VMEM((groups * capacity, units), outgoing.dtype),
            pltpu.VMEM((width, units), gate.dtype),
            pltpu.VMEM((width, units), up.dtype),
            pltpu.VMEM((units, width), down.dtype),
            pltpu.VMEM((chips * n, capacity, width), outgoing.dtype),
            pltpu.VMEM((apart, capacity, width), outgoing.dtype),
            pltpu.VMEM((n, capacity, width), outgoing.dtype),
            pltpu.SemaphoreType.DMA((3,)),
            pltpu.SemaphoreType.DMA((n,)),
            pltpu.SemaphoreType.DMA((max(1, chips - 1) * n,)),
            pltpu.SemaphoreType.DMA((groups * n,)),
            pltpu.SemaphoreType.DMA((groups * n,)),
            pltpu.SemaphoreType.DMA((chips * n,)),
            pltpu.SemaphoreType.DMA((chips * n,)),
            pltpu.SemaphoreType.DMA((apart,)),
            pltpu.SemaphoreType.DMA((apart,)),
            pltpu.SemaphoreType.DMA((n,)),
            pltpu.SemaphoreType.DMA((n,)),
        ],
        compiler_params=pltpu.CompilerParams(
            collective_id=1, has_side_effects=True, vmem_limit_bytes=60 * 1024 * 1024
        ),
        name="dispatch",
    )(outgoing, gate, up, down)


def shards(
    queries,
    keys,
    values,
    key_bias,
    residual,
    out_weight,
    norm_gain,
    routes,
    route_weights,
    gate_weight,
    up_weight,
    down_weight,
):
    sp_count = lax.axis_size("sp")
    attended = attend(queries, keys, values, key_bias)
    token_heads = lax.all_to_all(attended, "tp", split_axis=0, concat_axis=1, tiled=True)
    projected = jnp.dot(token_heads, out_weight, preferred_element_type=jnp.float32)
    stream = (residual.astype(jnp.float32) + projected).astype(jnp.bfloat16).astype(jnp.float32)
    normed = (
        stream * lax.rsqrt(jnp.mean(stream * stream, axis=-1, keepdims=True) + epsilon) * norm_gain
    ).astype(jnp.bfloat16)
    token_count = residual.shape[0]
    width_model = residual.shape[1]
    capacity = max(2, 5 * token_count * TOP // (4 * sp_count))
    flat_routes = routes.reshape(-1)
    onehot = (flat_routes[:, None] == lax.iota(jnp.int32, sp_count)[None, :]).astype(jnp.int32)
    before = jnp.cumsum(onehot, axis=0) - onehot
    slot_of = flat_routes * capacity + jnp.sum(before * onehot, axis=1)
    select = (slot_of[:, None] == lax.iota(jnp.int32, sp_count * capacity)[None, :]).astype(
        jnp.bfloat16
    )
    placing = jnp.sum(select.reshape(token_count, TOP, sp_count * capacity), axis=1)
    outgoing = jnp.einsum("ts,td->sd", placing, normed, preferred_element_type=jnp.float32).astype(
        jnp.bfloat16
    )
    returned = dispatch(
        outgoing.reshape(sp_count, capacity, width_model),
        gate_weight[0],
        up_weight[0],
        down_weight[0],
    ).reshape(-1, width_model)
    picked = jnp.dot(select, returned, preferred_element_type=jnp.float32).reshape(
        token_count, TOP, width_model
    )
    routed = jnp.sum(picked * route_weights[:, :, None], axis=1)
    return (stream + routed).astype(jnp.bfloat16)


def solution(mesh):
    return jax.shard_map(
        shards,
        mesh=mesh,
        in_specs=(
            P("sp", "tp"),
            P("sp", "tp"),
            P("sp", "tp"),
            P("sp", "tp"),
            P(("sp", "tp"), None),
            P(),
            P(),
            P(("sp", "tp"), None),
            P(("sp", "tp"), None),
            P("sp", None, "tp"),
            P("sp", None, "tp"),
            P("sp", "tp", None),
        ),
        out_specs=P(("sp", "tp"), None),
        check_vma=False,
    )
```
